32 devices in a mesh: ep: 16 (over z, y, x), tp: 2 (over core).
Axes of the slice: x: 2, y: 2, z: 4, core: 2. Of those that a mesh axis runs over, the one named last changes fastest.
Arguments:
- tokens: bfloat16 [256, 2048], P('ep'), may hold values from -6 to 6
- mix_gain: float32 [2048], replicated, may hold values from 0.1 to 1.9
- query_weight: bfloat16 [2048, 1024], P('ep', 'tp'), may hold values from -0.125 to 0.125
- forget_weight: bfloat16 [2048, 1024], P('ep', 'tp'), may hold values from -0.125 to 0.125
- input_weight: bfloat16 [2048, 1024], P('ep', 'tp'), may hold values from -0.125 to 0.125
- lower_bound: float32 [1024], P('tp'), may hold values from 0 to 0.9
- head_gain: float32 [1024], P('tp'), may hold values from 0.1 to 1.9
- out_weight: bfloat16 [1024, 2048], P('tp', 'ep'), may hold values from -0.1875 to 0.1875
- state: float32 [256, 8, 128, 128], P('ep', 'tp'), may hold values from -4 to 4
- ffn_gain: float32 [2048], replicated, may hold values from 0.1 to 1.9
- route_ids: int32 [256, 2], P('ep'), may hold values from 0 to 7, all different within a row; in each aligned block of 16 rows (0 to 15, 16 to 31, ...) at most 6 rows name the same one
- route_weights: float32 [256, 2], P('ep'), may hold values from 0.25 to 1
- expert_gate: bfloat16 [16, 2048, 2048], P('ep', None, 'tp'), may hold values from -0.125 to 0.125
- expert_up: bfloat16 [16, 2048, 2048], P('ep', None, 'tp'), may hold values from -0.125 to 0.125
- expert_down: bfloat16 [16, 2048, 2048], P('ep', 'tp'), may hold values from -0.09375 to 0.09375
Outputs:
- mixed_out: bfloat16 [256, 2048], P('ep', 'tp')
- new_state: float32 [256, 8, 128, 128], P('ep', 'tp')
The draws below stay inside these ranges and needn't reach their ends.
Inputs may be any that keep to these rules, and one draw needn't show every extreme that they name: `route_ids`: each row names 2 different experts; among the rows of one device no expert is named by more than 6 rows, a bound that some block reaches of them.
All inputs are finite; a program needn't handle non-finite values.
Results may differ from the reference program's by a relative error of at most 0.015.
Values may be sent and summed in bfloat16 or wider, within the bound.
A program may use at most 64 MiB of HBM per device.

```python
import math
import jax
import jax.numpy as jnp
import numpy as np
from jax import lax

D = 2048
HEADS = 8
HEAD_DIM = 128
FF_E = 4096
EXPERTS = 8
TOP = 2
SEQ_DEV = 16
CAP = 6
SEQS = 256
SPAN = 2
N_EP = 16
N_TP = 2


def steps_of(own_key, extent, shards, smallest, high):
    def one(position, shards_of):
        steps = jax.random.uniform(jax.random.fold_in(jax.random.fold_in(own_key, 6), position), (shards_of,), jnp.float32, smallest / len(shards), high / len(shards))
        return jnp.repeat(jnp.exp(steps), extent[position] // shards_of).reshape((-1,) + (1,) * (len(extent) - position - 1))

    level = one(*shards[0])
    for cut in shards[1:]:
        level = level * one(*cut)
    return level


def assign_block(own_key, own, number, rows, count, top, bound, slope):
    ranking = jax.random.permutation(own_key, count)
    packed, ordinary = portions_of(count, rows * top, bound, slope, True), portions_of(count, rows * top, bound, slope, False)
    places = jnp.arange(count)

    def named(tallies, rotation):
        used = int((tallies > 0).sum())
        fixed = max(1, used // 4)
        moved = fixed + (places - fixed + rotation * (used - fixed)) % max(1, count - fixed)
        return jnp.zeros((count,), jnp.int32).at[ranking[jnp.where(places < fixed, places, moved)]].set(jnp.asarray(tallies, jnp.int32))

    tallies = jnp.where(number % 4 == 0, named(packed, number // 4), named(ordinary, number - number // 4 - 1))
    mixed = jax.random.permutation(jax.random.fold_in(own, 3), count)
    giver, receiver = mixed[0:count // 2 * 2:2], mixed[1:count // 2 * 2:2]
    margin = jnp.minimum(tallies[giver] - 1, bound - tallies[receiver]) // 2
    margin = jnp.where((giver == ranking[0]) | (receiver == ranking[0]) | (tallies[receiver] == 0), 0, jnp.maximum(margin, 0))
    moved = jax.random.randint(jax.random.fold_in(own, 4), (count // 2,), 0, 1 << 20) % (margin + 1)
    tallies = tallies.at[giver].add(-moved).at[receiver].add(moved)
    labels = jnp.searchsorted(jnp.cumsum(tallies), jnp.arange(rows * top), side="right").astype(jnp.int32)
    grid = labels.reshape(top, rows).T
    grid = grid[jax.random.permutation(jax.random.fold_in(own, 1), rows)]
    rotation = jax.random.randint(jax.random.fold_in(own, 2), (rows, 1), 0, top)
    return jnp.take_along_axis(grid, (jnp.arange(top)[None, :] + rotation) % top, axis=1)


def portions_of(count, total, reach, slope, full):
    weights = [(1 << 20) // math.isqrt(rank ** slope) + 1 for rank in range(1, count + 1)]
    largest = reach if full else min(reach, max(-(-total // count), total * weights[0] // sum(weights)))
    least = 1 if total - largest >= count - 1 else 0
    counts, rest = [largest] + [least] * (count - 1), total - largest - least * (count - 1)
    while rest > 0:
        movable = [i for i in range(1, count) if counts[i] < largest] or [i for i in range(1, count) if counts[i] < reach]
        mass, budget = sum([weights[i] for i in movable]), rest
        for i in movable:
            extra = min(reach - counts[i], max(1, budget * weights[i] // mass), rest)
            counts[i] = counts[i] + extra
            rest = rest - extra
    return np.array(counts)


def centred(own_key, extent, spread, limit, shards=(), held_as=jnp.bfloat16):
    values = spread * jax.random.normal(own_key, extent, jnp.float32)
    if shards:
        values = values * steps_of(own_key, extent, shards, -0.22, 0.18)
    return jnp.clip(values, -limit, limit).astype(held_as)


def setup_inputs(seed: int = 0) -> dict:
    arg_keys = jax.random.split(jax.random.key(seed), 16)
    tokens = centred(arg_keys[0], (SEQS, D), 1.0, 6.0, ((0, 16),))
    mix_gain = jnp.clip(1.0 + 0.18 * jax.random.normal(arg_keys[1], (D,), jnp.float32), 0.1, 1.9)
    query_weight = centred(arg_keys[2], (D, HEADS * HEAD_DIM), D ** -0.5, 0.125, ((0, 16), (1, 2)))
    forget_weight = centred(arg_keys[3], (D, HEADS * HEAD_DIM), D ** -0.5, 0.125, ((0, 16), (1, 2)))
    input_weight = centred(arg_keys[4], (D, HEADS * HEAD_DIM), D ** -0.5, 0.125, ((0, 16), (1, 2)))
    lower_bound = jnp.clip(0.9 * jax.random.uniform(arg_keys[5], (HEADS * HEAD_DIM,), jnp.float32) ** steps_of(arg_keys[5], (HEADS * HEAD_DIM,), ((0, 2),), -0.2, 0.2), 0.0, 0.9)
    head_gain = jnp.clip(1.0 + 0.18 * jax.random.normal(arg_keys[6], (HEADS * HEAD_DIM,), jnp.float32), 0.1, 1.9)
    out_weight = centred(arg_keys[7], (HEADS * HEAD_DIM, D), (HEADS * HEAD_DIM) ** -0.5, 0.1875, ((0, 2), (1, 16)))
    state = centred(arg_keys[8], (SEQS, HEADS, HEAD_DIM, HEAD_DIM), 0.5, 4.0, ((0, 16), (1, 2)), jnp.float32)
    ffn_gain = jnp.clip(1.0 + 0.18 * jax.random.normal(arg_keys[9], (D,), jnp.float32), 0.1, 1.9)
    route_ids_keys = jax.random.split(jax.random.fold_in(arg_keys[10], 1), SEQS // SEQ_DEV)
    route_ids_turns = jax.random.permutation(jax.random.fold_in(arg_keys[10], 3), SEQS // SEQ_DEV)
    route_ids = jax.vmap(lambda own, number: assign_block(jax.random.fold_in(arg_keys[10], 2), own, number, SEQ_DEV, EXPERTS, TOP, CAP, 2))(route_ids_keys, route_ids_turns).reshape((SEQS, TOP))
    route_weights = jnp.clip(0.25 + 0.75 * jax.random.uniform(arg_keys[11], (SEQS, TOP), jnp.float32) ** steps_of(arg_keys[11], (SEQS, TOP), ((0, 16),), -0.2, 0.2), 0.25, 1.0)
    expert_gate = centred(arg_keys[12], (EXPERTS * SPAN, D, FF_E // SPAN), D ** -0.5, 0.125, ((0, 16), (2, 2)))
    expert_up = centred(arg_keys[13], (EXPERTS * SPAN, D, FF_E // SPAN), D ** -0.5, 0.125, ((0, 16), (2, 2)))
    expert_down = centred(arg_keys[14], (EXPERTS * SPAN, FF_E // SPAN, D), FF_E ** -0.5, 0.09375, ((0, 16), (1, 2)))
    return {"tokens": tokens, "mix_gain": mix_gain, "query_weight": query_weight, "forget_weight": forget_weight, "input_weight": input_weight, "lower_bound": lower_bound, "head_gain": head_gain, "out_weight": out_weight, "state": state, "ffn_gain": ffn_gain, "route_ids": route_ids, "route_weights": route_weights, "expert_gate": expert_gate, "expert_up": expert_up, "expert_down": expert_down}


epsilon = 1e-06

def rms_scale(values_in, gain_vec):
    return values_in * lax.rsqrt(lax.optimization_barrier(jnp.mean(values_in * values_in, axis=-1, keepdims=True)) + epsilon) * gain_vec

def reference(tokens, mix_gain, query_weight, forget_weight, input_weight, lower_bound, head_gain, out_weight, state, ffn_gain, route_ids, route_weights, expert_gate, expert_up, expert_down):
    batch_size = tokens.shape[0]
    residual = tokens.astype(jnp.float32)
    normed = rms_scale(residual, mix_gain).astype(jnp.bfloat16)
    queries = jnp.dot(normed, query_weight, preferred_element_type=jnp.float32).reshape(batch_size, HEADS, HEAD_DIM)
    forget_pre = jnp.dot(normed, forget_weight, preferred_element_type=jnp.float32)
    fresh_values = jnp.dot(normed, input_weight, preferred_element_type=jnp.float32).reshape(batch_size, HEADS, HEAD_DIM)
    forget = (lower_bound + (1.0 - lower_bound) * jax.nn.sigmoid(forget_pre)).reshape(batch_size, HEADS, HEAD_DIM)
    new_state = forget[..., None] * state + (1.0 - forget)[..., None] * fresh_values[:, :, None, :]
    readout = jnp.einsum('shk,shkv->shv', queries, new_state, precision=lax.Precision.HIGHEST)
    readout = rms_scale(readout, head_gain.reshape(HEADS, HEAD_DIM))
    heads_out = readout.reshape(batch_size, HEADS * HEAD_DIM).astype(jnp.bfloat16)
    group_cols = HEADS * HEAD_DIM // N_TP
    mixer_sum = jnp.zeros((batch_size, D), jnp.float32)
    for group in range(N_TP):
        product = jnp.dot(heads_out[:, group * group_cols:(group + 1) * group_cols], out_weight[group * group_cols:(group + 1) * group_cols], preferred_element_type=jnp.float32).astype(jnp.bfloat16)
        product = lax.optimization_barrier(product)
        mixer_sum = mixer_sum + product.astype(jnp.float32)
    after_mixer = (residual + mixer_sum).astype(jnp.bfloat16)
    ffn_in = rms_scale(after_mixer.astype(jnp.float32), ffn_gain).astype(jnp.bfloat16)
    expert_span = N_EP // EXPERTS
    span_cols = FF_E // expert_span
    gate_full = expert_gate.reshape(EXPERTS, expert_span, D, span_cols).transpose(0, 2, 1, 3).reshape(EXPERTS, D, FF_E)
    up_full = expert_up.reshape(EXPERTS, expert_span, D, span_cols).transpose(0, 2, 1, 3).reshape(EXPERTS, D, FF_E)
    down_full = expert_down.reshape(EXPERTS, FF_E, D)
    pair_count = SEQ_DEV * TOP
    flat_ids = route_ids.reshape(N_EP, pair_count).astype(jnp.int32)
    onehot = (flat_ids[..., None] == jnp.arange(EXPERTS, dtype=jnp.int32)).astype(jnp.int32)
    slot_rank = lax.optimization_barrier(jnp.sum((jnp.cumsum(onehot, axis=1).astype(jnp.int32) - onehot) * onehot, axis=-1)).astype(jnp.int32)
    slot_index = (jnp.arange(N_EP, dtype=jnp.int32)[:, None] * CAP + slot_rank).reshape(-1).astype(jnp.int32)
    expert_index = flat_ids.reshape(-1)
    token_index = (jnp.arange(batch_size * TOP, dtype=jnp.int32) // TOP).astype(jnp.int32)
    slot_table = jnp.full((EXPERTS, N_EP * CAP), batch_size, dtype=jnp.int32).at[expert_index, slot_index].set(token_index)
    padded_rows = jnp.concatenate([ffn_in, jnp.zeros((1, D), jnp.bfloat16)], axis=0)

    def expert_step(inputs):
        gate_w, up_w, down_w, table_row = inputs
        slot_rows = padded_rows[table_row]
        gate_pre = jnp.dot(slot_rows, gate_w, preferred_element_type=jnp.float32)
        up_pre = jnp.dot(slot_rows, up_w, preferred_element_type=jnp.float32)
        hidden = (jax.nn.silu(gate_pre) * up_pre).astype(jnp.bfloat16)
        return jnp.dot(hidden, down_w, preferred_element_type=jnp.float32)
    expert_out = lax.map(expert_step, (gate_full, up_full, down_full, slot_table))
    picked = expert_out[expert_index, slot_index].reshape(batch_size, TOP, D)
    expert_mix = lax.optimization_barrier(jnp.sum(picked * route_weights[:, :, None], axis=1))
    mixed_out = (after_mixer.astype(jnp.float32) + expert_mix).astype(jnp.bfloat16)
    return (mixed_out, new_state)
```

```python
import functools

import jax
import jax.numpy as jnp
from jax import lax
from jax.experimental import pallas as pl
from jax.experimental.pallas import tpu as pltpu
from jax.sharding import PartitionSpec as P

MESH = pl.DeviceIdType.MESH
PLANE = 4
EXPERTS = 8
TOP = 2


epsilon = 1e-06


def rms_scale(values_in, gain_vec):
    return (
        values_in
        * lax.rsqrt(jnp.mean(values_in * values_in, axis=-1, keepdims=True) + epsilon)
        * gain_vec
    )


def slot_ranks(block_ids, expert_count):
    onehot = (block_ids[..., None] == jnp.arange(expert_count, dtype=jnp.int32)).astype(jnp.int32)
    before = jnp.cumsum(onehot, axis=1) - onehot
    return jnp.sum(before * onehot, axis=-1)


def gathered_shards(
    tokens,
    mix_gain,
    query_weight,
    forget_weight,
    input_weight,
    lower_bound,
    head_gain,
    out_weight,
    state,
    ffn_gain,
    route_ids,
    route_weights,
    expert_gate,
    expert_up,
    expert_down,
):
    seq_dev = tokens.shape[0]
    model_width = tokens.shape[1]
    ep_count = lax.axis_size("ep")
    residual = tokens.astype(jnp.float32)
    normed = rms_scale(residual, mix_gain).astype(jnp.bfloat16)
    head_count = state.shape[1]
    head_size = state.shape[2]
    proj_width = query_weight.shape[1]
    pieces = (
        lax.all_gather(query_weight, "ep", axis=0, tiled=True),
        lax.all_gather(forget_weight, "ep", axis=0, tiled=True),
        lax.all_gather(input_weight, "ep", axis=0, tiled=True),
    )
    queries, forget_pre, fresh_values = tuple(
        (jnp.dot(normed, weight_rows, preferred_element_type=jnp.float32) for weight_rows in pieces)
    )
    forget = (lower_bound + (1.0 - lower_bound) * jax.nn.sigmoid(forget_pre)).reshape(
        seq_dev, head_count, head_size
    )
    queries = queries.reshape(seq_dev, head_count, head_size)
    fresh_values = fresh_values.reshape(seq_dev, head_count, head_size)
    new_state = forget[..., None] * state + (1.0 - forget)[..., None] * fresh_values[:, :, None, :]
    readout = jnp.einsum("shk,shkv->shv", queries, new_state, precision=lax.Precision.HIGHEST)
    readout = rms_scale(readout, head_gain.reshape(head_count, head_size))
    heads_out = readout.reshape(seq_dev, proj_width).astype(jnp.bfloat16)
    partial_mix = jnp.dot(
        heads_out,
        lax.all_gather(out_weight, "ep", axis=1, tiled=True),
        preferred_element_type=jnp.float32,
    )
    mixer_sum = lax.psum(partial_mix.astype(jnp.bfloat16), "tp").astype(jnp.float32)
    after_mixer = (residual + mixer_sum).astype(jnp.bfloat16)
    ffn_in = rms_scale(after_mixer.astype(jnp.float32), ffn_gain).astype(jnp.bfloat16)
    capacity = 3 * seq_dev // 8
    expert_span = ep_count // EXPERTS
    half_width = model_width // lax.axis_size("tp")
    own_columns = lax.dynamic_slice_in_dim(
        after_mixer, lax.axis_index("tp") * half_width, half_width, 1
    ).astype(jnp.float32)
    gate_slice = expert_gate[0]
    up_slice = expert_up[0]
    down_slice = expert_down[0]
    slot_iota = jnp.arange(capacity, dtype=jnp.int32)
    own_rank = slot_ranks(route_ids.reshape(1, seq_dev * TOP), EXPERTS).reshape(seq_dev, TOP)
    expert_iota = jnp.arange(EXPERTS, dtype=jnp.int32)
    chosen = (route_ids[:, :, None, None] == expert_iota[None, None, :, None]) & (
        own_rank[:, :, None, None] == slot_iota[None, None, None, :]
    )
    dispatch = jnp.any(chosen, axis=1).astype(jnp.bfloat16)
    combine = jnp.sum(chosen.astype(jnp.float32) * route_weights[:, :, None, None], axis=1)
    outgoing = jnp.einsum(
        "tec,td->ecd", dispatch, ffn_in, preferred_element_type=jnp.float32
    ).astype(jnp.bfloat16)
    outgoing = jnp.broadcast_to(
        outgoing[:, None], (EXPERTS, expert_span, capacity, model_width)
    ).reshape(ep_count, capacity, model_width)
    slot_rows = lax.all_to_all(outgoing, "ep", split_axis=0, concat_axis=0, tiled=True)
    gate_pre = jnp.einsum(
        "...d,df->...f", slot_rows, gate_slice, preferred_element_type=jnp.float32
    )
    up_pre = jnp.einsum("...d,df->...f", slot_rows, up_slice, preferred_element_type=jnp.float32)
    hidden = (jax.nn.silu(gate_pre) * up_pre).astype(jnp.bfloat16)
    partial_out = jnp.einsum(
        "...f,fd->...d", hidden, down_slice, preferred_element_type=jnp.float32
    )
    reduced = lax.psum_scatter(
        partial_out.astype(jnp.bfloat16), "tp", scatter_dimension=2, tiled=True
    ).astype(jnp.float32)
    returned = lax.all_to_all(
        reduced.astype(jnp.bfloat16), "ep", split_axis=0, concat_axis=0, tiled=True
    ).astype(reduced.dtype)
    expert_out = jnp.sum(returned.reshape(EXPERTS, expert_span, capacity, half_width), axis=1)
    expert_mix = jnp.einsum("tec,ecd->td", combine, expert_out, precision=lax.Precision.HIGHEST)
    mixed_out = (own_columns + expert_mix).astype(jnp.bfloat16)
    return (mixed_out, new_state)


X, P0, S0, W, H, M, O, SHARE, TRADE, R, PHASES = 0, 1, 4, 7, 8, 9, 10, 11, 12, 13, 14


def layer_kernel(
    n,
    m,
    capacity,
    tokens_hbm,
    mix_gain_hbm,
    query_hbm,
    forget_hbm,
    input_hbm,
    bound_hbm,
    head_gain_hbm,
    out_hbm,
    state_hbm,
    ffn_gain_hbm,
    ids_hbm,
    weights_hbm,
    gate_hbm,
    up_hbm,
    down_hbm,
    mixed_ref,
    state_buf,
    tokens_ref,
    mix_gain_ref,
    parts_ref,
    bound_ref,
    head_gain_ref,
    out_ref,
    ffn_gain_ref,
    ids_ref,
    weights_ref,
    gate_buf,
    up_buf,
    down_buf,
    state_low,
    x_send,
    x_recv,
    p_send,
    p_recv,
    s_send,
    s_recv,
    out_all,
    h_send,
    h_recv,
    m_send,
    m_recv,
    after_buf,
    ffn_buf,
    o_send,
    o_recv,
    hidden_buf,
    c_send,
    c_recv,
    r_send,
    r_recv,
    own_buf,
    local_sem,
    send_sem,
    recv_sem,
    row_sem,
):
    me = lax.axis_index("ep")
    core = lax.axis_index("tp")
    twin = 1 - core
    f32, bf16 = jnp.float32, jnp.bfloat16
    seqs, width = tokens_ref.shape
    rows, proj = parts_ref.shape[1:]
    heads = state_buf.shape[1]
    size = state_buf.shape[2]
    span = n // EXPERTS
    half = width // m

    barrier = pltpu.get_barrier_semaphore()

    def greet(i, carry):
        peer = lax.rem(me + i, n)
        for other in range(m):

            @pl.when((peer != me) | (core != other))
            def _():
                pl.semaphore_signal(barrier, inc=1, device_id=(peer, other), device_id_type=MESH)

        return carry

    lax.fori_loop(0, n, greet, 0)

    pairs = [
        (tokens_hbm, tokens_ref),
        (mix_gain_hbm, mix_gain_ref),
        (ids_hbm, ids_ref),
        (weights_hbm, weights_ref),
        (query_hbm, parts_ref.at[0]),
        (forget_hbm, parts_ref.at[1]),
        (input_hbm, parts_ref.at[2]),
        (out_hbm, out_ref),
        (bound_hbm, bound_ref),
        (head_gain_hbm, head_gain_ref),
        (ffn_gain_hbm, ffn_gain_ref),
        (state_hbm, state_buf),
        (gate_hbm.at[0], gate_buf),
        (up_hbm.at[0], up_buf),
        (down_hbm.at[0], down_buf),
    ]
    loads = [
        pltpu.make_async_copy(far, near, local_sem.at[i]) for i, (far, near) in enumerate(pairs)
    ]
    for load in loads:
        load.start()

    plane = PLANE
    lines = n // plane
    level, place = lax.div(me, plane), lax.rem(me, plane)
    counts = {"all": n, "line": lines, "plane": plane}

    def partner(group, i):
        if group == "plane":
            return level * plane + lax.rem(place + i, plane)
        return lax.rem(me + i * (plane if group == "line" else 1), n)

    def remote(phase, peer, other, source, target, arrival=None):
        return pltpu.make_async_remote_copy(
            src_ref=source,
            dst_ref=target,
            send_sem=send_sem.at[phase],
            recv_sem=recv_sem.at[phase] if arrival is None else arrival,
            device_id=(peer, other),
            device_id_type=MESH,
        )

    def send_all(phase, shift, source, target, group="all"):
        other = lax.rem(core + shift, m)

        def step(i, carry):
            peer = partner(group, i)
            remote(phase, peer, other, source(peer), target(me)).start()
            return carry

        lax.fori_loop(0 if shift else 1, counts[group], step, 0)

    def received(phase, block):
        remote(phase, me, twin, block, block).wait_recv()

    def sent(phase, block):
        remote(phase, me, twin, block, block).wait_send()

    for load in loads[:4]:
        load.wait()
    residual = tokens_ref[...].astype(f32)
    normed = rms_scale(residual, mix_gain_ref[...]).astype(bf16)
    for peer in range(n):
        x_send[peer] = normed[:, peer * rows : (peer + 1) * rows]

    ids = ids_ref[...]
    routed = weights_ref[...]
    pad = -(-capacity // 8) * 8
    slots = EXPERTS * pad
    slot = lax.broadcasted_iota(jnp.int32, (slots, seqs), 0)
    first = jnp.where(slot // pad == ids[0:1, :], 1.0, 0.0)
    second = jnp.where(slot // pad == ids[1:2, :], 1.0, 0.0)
    named = first + second
    upper = jnp.where(
        lax.broadcasted_iota(jnp.int32, (seqs, seqs), 0)
        < lax.broadcasted_iota(jnp.int32, (seqs, seqs), 1),
        1.0,
        0.0,
    )
    before = jnp.dot(named.astype(bf16), upper.astype(bf16), preferred_element_type=f32)
    taken = jnp.where(jnp.abs(before - (slot % pad).astype(f32)) < 0.5, named, 0.0)
    combine = (taken * (first * routed[0:1, :] + second * routed[1:2, :])).T

    for load in loads[4:11]:
        load.wait()
    pl.semaphore_wait(barrier, n * m - 1)

    send_all(X, 0, lambda p: x_send.at[p], lambda p: x_recv.at[p])
    out_all[pl.ds(place, 1)] = out_ref[...][None]
    x_recv[pl.ds(me, 1)] = x_send[pl.ds(me, 1)]
    loads[11].wait()

    def lower(s, carry):
        state_low[s] = state_buf[s].astype(bf16)
        return carry

    lax.fori_loop(0, seqs, lower, 0)
    received(X, x_recv.at[pl.ds(0, n - 1)])

    gathered = x_recv[...].reshape(n * seqs, rows)
    for k in range(3):
        product = (
            jnp.dot(gathered, parts_ref[k], preferred_element_type=f32)
            .reshape(lines, plane, seqs, proj)
            .astype(bf16)
        )
        for q in range(plane):
            p_send[k, q] = product[:, q]
        send_all(
            P0 + k,
            0,
            lambda p, k=k: p_send.at[k, lax.rem(p, plane)],
            lambda p, k=k: p_recv.at[k, lax.rem(p, plane)],
            "plane",
        )
    for k in range(3):
        p_recv[k, pl.ds(place, 1)] = p_send[k, pl.ds(place, 1)]
        received(P0 + k, p_recv.at[k, pl.ds(0, plane - 1)])
        s_send[k] = sum(p_recv[k, q].astype(f32) for q in range(plane)).astype(bf16)
        send_all(
            S0 + k,
            0,
            lambda p, k=k: s_send.at[k, lax.div(p, plane)],
            lambda p, k=k: s_recv.at[k, lax.div(p, plane)],
            "line",
        )
    send_all(W, 0, lambda p: out_ref, lambda p: out_all.at[lax.rem(p, plane)], "plane")
    joined = []
    for k in range(3):
        s_recv[k, pl.ds(level, 1)] = s_send[k, pl.ds(level, 1)]
        received(S0 + k, s_recv.at[k, pl.ds(0, lines - 1)])
        joined.append(sum(s_recv[k, z].astype(f32) for z in range(lines)))
    queries, forget_pre, fresh = joined
    bound = bound_ref[...]
    forget = bound + (1.0 - bound) * jax.nn.sigmoid(forget_pre)

    scaled = (queries * forget).astype(bf16)
    rest = queries * (1.0 - forget)
    row_of = lax.broadcasted_iota(jnp.int32, (seqs, size), 0)
    for h in range(heads):
        cut = slice(h * size, (h + 1) * size)
        readout = jnp.sum(rest[:, cut], axis=-1, keepdims=True) * fresh[:, cut]
        for s in range(seqs):
            line = jnp.dot(scaled[:, cut], state_low[s, h], preferred_element_type=f32)
            readout = readout + jnp.where(row_of == s, line, 0.0)
        h_send[:, cut] = rms_scale(readout, head_gain_ref[:, cut]).astype(bf16)

    send_all(H, 0, lambda p: h_send, lambda p: h_recv.at[lax.div(p, plane)], "line")
    h_recv[pl.ds(level, 1)] = h_send[...][None]
    forget_columns = forget.T
    for s in range(seqs):
        for h in range(heads):
            keep = forget_columns[h * size : (h + 1) * size, s : s + 1]
            entering = fresh[s : s + 1, h * size : (h + 1) * size]
            state_buf[s, h] = keep * state_buf[s, h] + (1.0 - keep) * entering
    received(W, out_all.at[pl.ds(0, plane - 1)])
    received(H, h_recv.at[pl.ds(0, lines - 1)])
    every_head = h_recv[...].reshape(lines * seqs, proj)
    for q in range(plane):
        m_send[:, q] = (
            jnp.dot(every_head, out_all[q], preferred_element_type=f32)
            .reshape(lines, seqs, rows)
            .astype(bf16)
        )
    for shift in range(m):
        send_all(
            M,
            shift,
            lambda p: m_send.at[lax.div(p, plane)],
            lambda p: m_recv.at[core * lines + lax.div(p, plane)],
            "line",
        )
    m_recv[pl.ds(core * lines + level, 1)] = m_send[pl.ds(level, 1)]
    received(M, m_recv.at[pl.ds(0, m * lines - 1)])
    mixer_sum = jnp.concatenate(
        [
            sum(m_recv[c * lines + z, q].astype(f32) for c in range(m))
            for z in range(lines)
            for q in range(plane)
        ],
        axis=1,
    )
    after = (residual + mixer_sum).astype(bf16).astype(f32)
    after_buf[...] = after
    ffn_buf[...] = rms_scale(after, ffn_gain_ref[...]).astype(bf16)
    own_cut = pl.ds(pl.multiple_of(core * half, 128), half)
    o_send[...] = (
        jnp.dot(taken.astype(bf16), ffn_buf[:, own_cut], preferred_element_type=f32)
        .reshape(EXPERTS, pad, half)
        .astype(bf16)
    )
    used = pl.ds(0, capacity)

    def give(i, carry):
        peer = partner("all", i)
        remote(
            O,
            peer,
            core,
            o_send.at[lax.div(peer, span), used],
            o_recv.at[core, me, used],
            row_sem.at[me],
        ).start()
        return carry

    lax.fori_loop(1, n, give, 0)
    o_recv[pl.ds(core, 1), pl.ds(me, 1)] = o_send[pl.ds(lax.div(me, span), 1)][None]

    def pass_on(i, carry):
        peer = partner("all", n - i)
        block = o_recv.at[core, peer, used]

        @pl.when(i > 0)
        def _():
            remote(O, me, twin, block, block, row_sem.at[peer]).wait_recv()

        remote(SHARE, me, twin, block, block).start()
        return carry

    lax.fori_loop(0, n, pass_on, 0)
    for load in loads[12:14]:
        load.wait()
    received(SHARE, o_recv.at[twin, pl.ds(0, n), used])
    slot_rows = [
        o_recv[c].astype(f32).reshape(n * pad, half).astype(bf16) for c in range(m)
    ]
    tile = 256

    def hidden_step(j, carry):
        cut = pl.ds(pl.multiple_of(j * tile, tile), tile)
        gate_pre, up_pre = (
            sum(
                jnp.dot(
                    slot_rows[c],
                    ref[c * half : (c + 1) * half, cut],
                    preferred_element_type=f32,
                )
                for c in range(m)
            )
            for ref in (gate_buf, up_buf)
        )
        hidden_buf[:, cut] = (jax.nn.silu(gate_pre) * up_pre).astype(bf16)
        return carry

    lax.fori_loop(0, gate_buf.shape[1] // tile, hidden_step, 0)
    hidden = hidden_buf[...]
    loads[14].wait()
    wide = 512

    def down_into(side, target):
        for j in range(half // wide):
            cut = pl.ds(j * wide, wide)
            from_cut = pl.ds(pl.multiple_of(side * half + j * wide, wide), wide)
            target[:, :, cut] = (
                jnp.dot(hidden, down_buf[:, from_cut], preferred_element_type=f32)
                .reshape(n, pad, wide)
                .astype(target.dtype)
            )

    down_into(twin, c_send)
    remote(TRADE, me, twin, c_send, c_recv).start()
    down_into(core, own_buf)
    received(TRADE, c_recv)
    r_send[...] = (own_buf[...] + c_recv[...].astype(f32)).astype(bf16)

    def send_back(i, carry):
        peer = partner("all", i)
        remote(R, peer, core, r_send.at[peer, used], r_recv.at[me, used]).start()
        return carry

    lax.fori_loop(1, n, send_back, 0)
    r_recv[pl.ds(me, 1)] = r_send[pl.ds(me, 1)]

    sent(X, x_send.at[pl.ds(0, n - 1)])
    sent(W, out_all.at[pl.ds(0, plane - 1)])
    for k in range(3):
        sent(P0 + k, p_send.at[k, pl.ds(0, plane - 1)])
        sent(S0 + k, s_send.at[k, pl.ds(0, lines - 1)])
    sent(H, h_recv.at[pl.ds(0, lines - 1)])
    sent(M, m_recv.at[pl.ds(0, m * lines - 1)])
    sent(O, r_recv.at[pl.ds(0, n - 1), used])
    sent(SHARE, o_recv.at[core, pl.ds(0, n), used])
    sent(TRADE, c_send)

    received(R, r_recv.at[pl.ds(0, n - 1), used])
    real = lax.broadcasted_iota(jnp.int32, (pad, half), 0) < capacity
    expert_out = jnp.concatenate(
        [
            jnp.where(real, sum(r_recv[e * span + k].astype(f32) for k in range(span)), 0.0)
            for e in range(EXPERTS)
        ],
        axis=0,
    )
    expert_mix = jnp.dot(
        combine, expert_out, preferred_element_type=f32, precision=lax.Precision.HIGHEST
    )
    own = after_buf[:, own_cut]
    mixed_ref[...] = (own + expert_mix).astype(bf16)
    sent(R, r_send.at[pl.ds(0, n - 1), used])


def exchanged_shards(
    n,
    m,
    tokens,
    mix_gain,
    query_weight,
    forget_weight,
    input_weight,
    lower_bound,
    head_gain,
    out_weight,
    state,
    ffn_gain,
    route_ids,
    route_weights,
    expert_gate,
    expert_up,
    expert_down,
):
    seqs, width = tokens.shape
    rows, proj = query_weight.shape
    columns = out_weight.shape[1]
    hidden = expert_gate.shape[2]
    half = width // m
    f32, bf16 = jnp.float32, jnp.bfloat16
    vmem, far = pl.BlockSpec(memory_space=pltpu.VMEM), pl.BlockSpec(memory_space=pltpu.HBM)
    lines = n // PLANE
    pad = -(-(3 * seqs // 8) // 8) * 8
    mixed_out, new_state = pl.pallas_call(
        functools.partial(layer_kernel, n, m, 3 * seqs // 8),
        out_shape=(
            pltpu.VMEM((seqs, half), bf16),
            pltpu.VMEM(state.shape, f32),
        ),
        in_specs=[far] * 15,
        out_specs=(vmem, vmem),
        scratch_shapes=[
            pltpu.VMEM((seqs, width), bf16),
            pltpu.VMEM((1, width), f32),
            pltpu.VMEM((3, rows, proj), bf16),
            pltpu.VMEM((1, proj), f32),
            pltpu.VMEM((1, proj), f32),
            pltpu.VMEM((proj, columns), bf16),
            pltpu.VMEM((1, width), f32),
            pltpu.VMEM((TOP, seqs), jnp.int32),
            pltpu.VMEM((TOP, seqs), f32),
            pltpu.VMEM(expert_gate.shape[1:], bf16),
            pltpu.VMEM(expert_up.shape[1:], bf16),
            pltpu.VMEM(expert_down.shape[1:], bf16),
            pltpu.VMEM(state.shape, bf16),
            pltpu.VMEM((n, seqs, rows), bf16),
            pltpu.VMEM((n, seqs, rows), bf16),
            pltpu.VMEM((3, PLANE, lines, seqs, proj), bf16),
            pltpu.VMEM((3, PLANE, lines, seqs, proj), bf16),
            pltpu.VMEM((3, lines, seqs, proj), bf16),
            pltpu.VMEM((3, lines, seqs, proj), bf16),
            pltpu.VMEM((PLANE, proj, columns), bf16),
            pltpu.VMEM((seqs, proj), bf16),
            pltpu.VMEM((lines, seqs, proj), bf16),
            pltpu.VMEM((lines, PLANE, seqs, columns), bf16),
            pltpu.VMEM((m * lines, PLANE, seqs, columns), bf16),
            pltpu.VMEM((seqs, width), f32),
            pltpu.VMEM((seqs, width), bf16),
            pltpu.VMEM((EXPERTS, pad, half), bf16),
            pltpu.VMEM((m, n, pad, half), bf16),
            pltpu.VMEM((n * pad, hidden), bf16),
            pltpu.VMEM((n, pad, half), bf16),
            pltpu.VMEM((n, pad, half), bf16),
            pltpu.VMEM((n, pad, half), bf16),
            pltpu.VMEM((n, pad, half), bf16),
            pltpu.VMEM((n, pad, half), f32),
            pltpu.SemaphoreType.DMA((15,)),
            pltpu.SemaphoreType.DMA((PHASES,)),
            pltpu.SemaphoreType.DMA((PHASES,)),
            pltpu.SemaphoreType.DMA((n,)),
        ],
        compiler_params=pltpu.CompilerParams(
            collective_id=0, has_side_effects=True, vmem_limit_bytes=60000 * 1024
        ),
    )(
        tokens,
        mix_gain[None],
        query_weight,
        forget_weight,
        input_weight,
        lower_bound[None],
        head_gain[None],
        out_weight,
        state,
        ffn_gain[None],
        route_ids.T,
        route_weights.T,
        expert_gate,
        expert_up,
        expert_down,
    )
    return (mixed_out, new_state)


def solution(mesh):
    n, m = mesh.shape["ep"], mesh.shape["tp"]

    def body(*args):
        rows = args[2].shape[0]
        columns = args[7].shape[1]
        if rows % 128 or columns % 128 or n % PLANE or m != 2:
            return gathered_shards(*args)
        return exchanged_shards(n, m, *args)

    return jax.shard_map(
        body,
        mesh=mesh,
        in_specs=(
            P("ep", None),
            P(),
            P("ep", "tp"),
            P("ep", "tp"),
            P("ep", "tp"),
            P("tp"),
            P("tp"),
            P("tp", "ep"),
            P("ep", "tp", None, None),
            P(),
            P("ep", None),
            P("ep", None),
            P("ep", None, "tp"),
            P("ep", None, "tp"),
            P("ep", "tp", None),
        ),
        out_specs=(P("ep", "tp"), P("ep", "tp", None, None)),
        check_vma=False,
    )
```
